32 devices in a mesh: sp: 8 (over z, y), tp: 4 (over x, core).
Axes of the slice: x: 2, y: 2, z: 4, core: 2. Of those that a mesh axis runs over, the one named last changes fastest.
Arguments:
- latent: bfloat16 [4096, 2048], P(('sp', 'tp')), may hold values from -6 to 6
- context: bfloat16 [512, 2048], P('sp'), may hold values from -6 to 6
- condition: float32 [2048], replicated, may hold values from -6 to 6
- context_condition: float32 [2048], replicated, may hold values from -6 to 6
- norm_gain: float32 [2048], replicated, may hold values from 0.1 to 1.9
- shift_weight: bfloat16 [2048, 2048], P('sp', 'tp'), may hold values from -0.21875 to 0.21875
- scale_weight: bfloat16 [2048, 2048], P('sp', 'tp'), may hold values from -0.21875 to 0.21875
- gate_weight: bfloat16 [2048, 2048], P('sp', 'tp'), may hold values from -0.21875 to 0.21875
- query_weight: bfloat16 [2048, 1024], P(None, 'tp'), may hold values from -1 to 1
- key_weight: bfloat16 [2048, 512], P(None, 'tp'), may hold values from -1 to 1
- value_weight: bfloat16 [2048, 512], P(None, 'tp'), may hold values from -0.125 to 0.125
- query_gain: float32 [64], replicated, may hold values from 0.1 to 7.8
- key_gain: float32 [64], replicated, may hold values from 0.1 to 7.8
- output_weight: bfloat16 [1024, 2048], replicated, may hold values from -1 to 1
Outputs:
- updated: bfloat16 [4096, 2048], P(('sp', 'tp'))
The draws below stay inside these ranges and needn't reach their ends.
All inputs are finite; a program needn't handle non-finite values.
Results may differ from the reference program's by a relative error of at most 0.012.
The reference program's roundings to bfloat16 on the way count: a program that leaves them out, or rounds other values in their place, can miss the bound.
Values may be sent and summed in bfloat16 or wider, within the bound.
A program may use at most 64 MiB of HBM per device.

```python
import math
import jax
import jax.numpy as jnp
from jax import lax

D = 2048
HQ = 16
KVH = 8
CHANNEL_SPAN = 64
GRID_W = 64
PREFIX_ITEMS = 512
HIDDEN_ITEMS = 4096


def query_base(key):
    return jax.random.truncated_normal(jax.random.fold_in(key, 101), -6.0, 6.0, (D, HQ * CHANNEL_SPAN), jnp.float32) * D ** (-0.5)


def draw_query_weight(key, part):
    return query_base(key).astype(jnp.bfloat16)


def draw_key_weight(key, part):
    fresh = jax.random.truncated_normal(jax.random.fold_in(key, 102), -6.0, 6.0, (D, KVH * CHANNEL_SPAN), jnp.float32) * D ** (-0.5)
    return fresh.astype(jnp.bfloat16)


def gain_draw(key, salt):
    return 3.0 * (1.0 + 0.18 * jax.random.truncated_normal(jax.random.fold_in(key, salt), -5.0, 5.0, (CHANNEL_SPAN,), jnp.float32))


def draw_query_gain(key, part):
    return gain_draw(key, 103)


def draw_key_gain(key, part):
    return gain_draw(key, 104)


def draw_output_weight(key, part):
    base = jax.random.truncated_normal(jax.random.fold_in(key, 105), -6.0, 6.0, (HQ * CHANNEL_SPAN, D), jnp.float32)
    return (base * (HQ * CHANNEL_SPAN) ** (-0.5)).astype(jnp.bfloat16)


def steps_of(own_key, dims, pieces, low, largest):
    loudness = 1.0
    for dim, parts in pieces:
        draws = jax.random.uniform(jax.random.fold_in(jax.random.fold_in(own_key, 6), dim), (parts,), jnp.float32, low / len(pieces), largest / len(pieces))
        loudness = loudness * jnp.repeat(jnp.exp(draws), dims[dim] // parts).reshape((-1,) + (1,) * (len(dims) - 1 - dim))
    return loudness


def scatter_about(key, extent, deviation, most, shards=(), kind=jnp.bfloat16):
    entries = deviation * jax.random.normal(key, extent, jnp.float32)
    if shards:
        entries = entries * steps_of(key, extent, shards, -0.22, 0.18)
    return jnp.clip(entries, -most, most).astype(kind)


def setup_inputs(seed: int = 0) -> dict:
    keys = jax.random.split(jax.random.key(seed), 15)
    latent = scatter_about(keys[0], (HIDDEN_ITEMS, D), 1.0, 6.0, ((0, 32),))
    context = scatter_about(keys[1], (PREFIX_ITEMS, D), 1.0, 6.0, ((0, 8),))
    condition = scatter_about(keys[2], (D,), 1.0, 6.0, (), jnp.float32)
    context_condition = scatter_about(keys[3], (D,), 1.0, 6.0, (), jnp.float32)
    norm_gain = jnp.clip(1.0 + 0.18 * jax.random.normal(keys[4], (D,), jnp.float32), 0.1, 1.9)
    shift_weight = scatter_about(keys[5], (D, D), (D // 3) ** -0.5, 0.21875, ((0, 8), (1, 4)))
    scale_weight = scatter_about(keys[6], (D, D), (D // 3) ** -0.5, 0.21875, ((0, 8), (1, 4)))
    gate_weight = scatter_about(keys[7], (D, D), (D // 3) ** -0.5, 0.21875, ((0, 8), (1, 4)))
    query_weight = draw_query_weight(jax.random.fold_in(keys[14], 71), 0)
    key_weight = draw_key_weight(jax.random.fold_in(keys[14], 71), 0)
    value_weight = scatter_about(keys[10], (D, KVH * CHANNEL_SPAN), D ** -0.5, 0.125, ((1, 4),))
    query_gain = draw_query_gain(jax.random.fold_in(keys[14], 71), 0)
    key_gain = draw_key_gain(jax.random.fold_in(keys[14], 71), 0)
    output_weight = draw_output_weight(jax.random.fold_in(keys[14], 71), 0)
    return {"latent": latent, "context": context, "condition": condition, "context_condition": context_condition, "norm_gain": norm_gain, "shift_weight": shift_weight, "scale_weight": scale_weight, "gate_weight": gate_weight, "query_weight": query_weight, "key_weight": key_weight, "value_weight": value_weight, "query_gain": query_gain, "key_gain": key_gain, "output_weight": output_weight}


epsilon = 1e-06
rope_base = 10000.0

def modulate(tok_rows, norm_gain, shift_row, scale_row):
    wide = tok_rows.astype(jnp.float32)
    normed = wide * lax.rsqrt(lax.optimization_barrier(jnp.mean(wide * wide, axis=-1, keepdims=True)) + epsilon)
    return (normed * norm_gain * (1.0 + scale_row) + shift_row).astype(jnp.bfloat16)

def headnorm(raw, gain, heads):
    field = raw.reshape(raw.shape[0], heads, -1)
    return field * lax.rsqrt(lax.optimization_barrier(jnp.mean(field * field, axis=-1, keepdims=True)) + epsilon) * gain

def rotate(field, places):
    count = field.shape[0]
    heads = field.shape[1]
    quarter = field.shape[2] // 4
    grid_row = (places // GRID_W).astype(jnp.float32)
    grid_col = (places % GRID_W).astype(jnp.float32)
    inverse = rope_base ** (-jnp.arange(quarter, dtype=jnp.float32) / quarter)
    angles = jnp.stack([grid_row[:, None] * inverse, grid_col[:, None] * inverse], axis=1)[:, None]
    cosine = jnp.cos(angles)
    sine = jnp.sin(angles)
    matcher_content_couples = field.reshape(count, heads, 2, 2, quarter)
    first = matcher_content_couples[:, :, :, 0]
    second = matcher_content_couples[:, :, :, 1]
    turned = jnp.stack([first * cosine - second * sine, second * cosine + first * sine], axis=3)
    return turned.reshape(count, heads, 4 * quarter)

def reference(latent, context, condition, context_condition, norm_gain, shift_weight, scale_weight, gate_weight, query_weight, key_weight, value_weight, query_gain, key_gain, output_weight):
    activated = jax.nn.silu(jnp.stack([condition, context_condition])).astype(jnp.bfloat16)
    shifts = jnp.dot(activated, shift_weight, preferred_element_type=jnp.float32)
    scales = jnp.dot(activated, scale_weight, preferred_element_type=jnp.float32)
    gates = jnp.dot(activated, gate_weight, preferred_element_type=jnp.float32)
    hidden = modulate(latent, norm_gain, shifts[0], scales[0])
    context_hidden = modulate(context, norm_gain, shifts[1], scales[1])
    places = jnp.arange(HIDDEN_ITEMS, dtype=jnp.int32)
    probe_entries = rotate(headnorm(jnp.dot(hidden, query_weight, preferred_element_type=jnp.float32), query_gain, HQ), places).astype(jnp.bfloat16)
    latent_keys = rotate(headnorm(jnp.dot(hidden, key_weight, preferred_element_type=jnp.float32), key_gain, KVH), places).astype(jnp.bfloat16)
    latent_values = jnp.dot(hidden, value_weight, preferred_element_type=jnp.float32).astype(jnp.bfloat16).reshape(HIDDEN_ITEMS, KVH, CHANNEL_SPAN)
    context_keys = headnorm(jnp.dot(context_hidden, key_weight, preferred_element_type=jnp.float32), key_gain, KVH).astype(jnp.bfloat16)
    context_values = jnp.dot(context_hidden, value_weight, preferred_element_type=jnp.float32).astype(jnp.bfloat16).reshape(PREFIX_ITEMS, KVH, CHANNEL_SPAN)
    matcher_pieces = jnp.concatenate([context_keys, latent_keys], axis=0).astype(jnp.float32)
    value_rows = jnp.concatenate([context_values, latent_values], axis=0).astype(jnp.float32)
    prefix_mapped = math.log(HIDDEN_ITEMS / (2.0 * PREFIX_ITEMS))
    similarity_offset = jnp.concatenate([jnp.full((PREFIX_ITEMS,), prefix_mapped, jnp.float32), jnp.zeros((HIDDEN_ITEMS,), jnp.float32)])
    group_size = HQ // KVH
    group_extent = math.gcd(HIDDEN_ITEMS, 256)
    grouped = probe_entries.reshape(HIDDEN_ITEMS // group_extent, group_extent, KVH, group_size, CHANNEL_SPAN)

    def one_block(probe_segment):
        similarity_matrix = jnp.einsum('dmvk,hmk->dmvh', probe_segment.astype(jnp.float32), matcher_pieces) * CHANNEL_SPAN ** (-0.5) + similarity_offset
        row_peak = lax.optimization_barrier(jnp.max(similarity_matrix, axis=-1, keepdims=True))
        shares = jnp.exp(similarity_matrix - row_peak)
        row_total = lax.optimization_barrier(jnp.sum(shares, axis=-1))
        rounded = lax.optimization_barrier(shares.astype(jnp.bfloat16)).astype(jnp.float32)
        weighted = jnp.einsum('qkgn,nkd->qkgd', rounded, value_rows)
        return (weighted / row_total[..., None]).astype(jnp.bfloat16)
    attended = lax.map(one_block, grouped).reshape(HIDDEN_ITEMS, HQ * CHANNEL_SPAN)
    projected = jnp.dot(attended, output_weight, preferred_element_type=jnp.float32)
    return (latent.astype(jnp.float32) + gates[0] * projected).astype(jnp.bfloat16)
```

```python
import functools
import math

import jax
import jax.numpy as jnp
from jax import lax
from jax.experimental import pallas as pl
from jax.experimental.pallas import tpu as pltpu
from jax.sharding import PartitionSpec as P

CHANNEL_SPAN = 64
GRID_W = 64
MESH = pl.DeviceIdType.MESH
VMEM = pl.BlockSpec(memory_space=pltpu.VMEM)
F32 = jnp.float32
BF16 = jnp.bfloat16

epsilon = 1e-06
rope_base = 10000.0


def greet(n_sp, n_tp):
    sp, tp = lax.axis_index("sp"), lax.axis_index("tp")
    barrier = pltpu.get_barrier_semaphore()
    for d in range(1, n_sp):
        pl.semaphore_signal(
            barrier, inc=1, device_id=(lax.rem(sp + d, n_sp), tp), device_id_type=MESH
        )
    for d in range(1, n_tp):
        pl.semaphore_signal(
            barrier, inc=1, device_id=(sp, lax.rem(tp + d, n_tp)), device_id_type=MESH
        )
    pl.semaphore_wait(barrier, n_sp + n_tp - 2)


def gather_kernel(
    n_sp, n_tp, latent, act, w_shift, w_scale, w_gate, lat_all, mods,
    part, parts, lat_send, lat_recv, sp_send, sp_recv, tp_send, tp_recv, own_sem,
):
    sp, tp = lax.axis_index("sp"), lax.axis_index("tp")
    part[...] = jnp.zeros_like(part)
    for i, w in enumerate((w_shift, w_scale, w_gate)):
        part[2 * i : 2 * i + 2, :] = jnp.dot(act[...], w[...], preferred_element_type=F32)[0:2]
    greet(n_sp, n_tp)
    sp_copies = []
    for d in range(1, n_sp):
        c = pltpu.make_async_remote_copy(
            src_ref=part, dst_ref=parts.at[sp], send_sem=sp_send.at[d - 1],
            recv_sem=sp_recv.at[d - 1], device_id=(lax.rem(sp + d, n_sp), tp), device_id_type=MESH,
        )
        c.start()
        sp_copies.append(c)
    lat_copies = []
    for d in range(1, n_tp):
        c = pltpu.make_async_remote_copy(
            src_ref=latent, dst_ref=lat_all.at[tp], send_sem=lat_send.at[d - 1],
            recv_sem=lat_recv.at[d - 1], device_id=(sp, lax.rem(tp + d, n_tp)), device_id_type=MESH,
        )
        c.start()
        lat_copies.append(c)
    own = pltpu.make_async_copy(latent, lat_all.at[tp], own_sem)
    own.start()
    parts[sp] = part[...]
    for c in sp_copies:
        c.wait()
    total = parts[0]
    for j in range(1, n_sp):
        total = total + parts[j]
    part[...] = total
    mods[tp] = total
    tp_copies = []
    for d in range(1, n_tp):
        c = pltpu.make_async_remote_copy(
            src_ref=part, dst_ref=mods.at[tp], send_sem=tp_send.at[d - 1],
            recv_sem=tp_recv.at[d - 1], device_id=(sp, lax.rem(tp + d, n_tp)), device_id_type=MESH,
        )
        c.start()
        tp_copies.append(c)
    own.wait()
    for c in tp_copies + lat_copies:
        c.wait()


def project_kernel(
    n_tp, lat_all, context, mods, norm_gain, w_q, w_k, w_v, q_gain, k_gain, cosine, sine,
    q_out, ctx_out, kv_out, hidden,
):
    own_rows = lat_all.shape[1]
    ctx_rows = context.shape[0]
    q_width = w_q.shape[1]
    kv_width = w_k.shape[1]
    kv_heads = kv_width // CHANNEL_SPAN
    q_heads = q_width // CHANNEL_SPAN
    group = q_heads // kv_heads
    span = mods.shape[2]

    def modulate(read, rows, row):
        total = jnp.zeros((rows, 1), F32)
        for t in range(n_tp):
            x = read(t).astype(F32)
            total = total + jnp.sum(x * x, axis=-1, keepdims=True)
        inv = lax.rsqrt(total / (n_tp * span) + epsilon)
        for t in range(n_tp):
            cols = slice(t * span, (t + 1) * span)
            x = read(t).astype(F32)
            y = x * inv * norm_gain[:, cols] * (1.0 + mods[t, 2 + row : 3 + row, :]) + mods[
                t, row : row + 1, :
            ]
            hidden[0:rows, cols] = y.astype(BF16)

    def headnorm(x, gain):
        width = x.shape[1]
        head = lax.broadcasted_iota(jnp.int32, x.shape, 1) // CHANNEL_SPAN
        sq = x * x
        scale = jnp.zeros_like(x)
        for h in range(width // CHANNEL_SPAN):
            s = jnp.sum(jnp.where(head == h, sq, 0.0), axis=-1, keepdims=True)
            scale = jnp.where(head == h, lax.rsqrt(s / CHANNEL_SPAN + epsilon), scale)
        return x * scale * gain

    def rotate(x, cos, sin):
        width = x.shape[1]
        full = x if width == 128 else jnp.concatenate([x, x], axis=1)
        lane = lax.broadcasted_iota(jnp.int32, full.shape, 1)
        other = jnp.where(lane % 32 < 16, pltpu.roll(full, 112, 1), pltpu.roll(full, 16, 1))
        return (full * cos + other * sin)[:, :width]

    piece = min(128, kv_width)
    modulate(lambda t: context[:, t * span : (t + 1) * span], ctx_rows, 1)
    h = hidden[0:ctx_rows, :]
    k = jnp.dot(h, w_k[...], preferred_element_type=F32)
    for c in range(0, kv_width, piece):
        ctx_out[:, c : c + piece] = headnorm(k[:, c : c + piece], k_gain[:, :piece]).astype(BF16)
    ctx_out[:, kv_width:] = jnp.dot(h, w_v[...], preferred_element_type=F32).astype(BF16)

    def tile(i, carry):
        modulate(lambda t: lat_all[i, :, t * span : (t + 1) * span], own_rows, 0)
        h = hidden[0:own_rows, :]
        rows = pl.ds(pl.multiple_of(i * own_rows, own_rows), own_rows)
        cos, sin = cosine[rows, :], sine[rows, :]
        k = jnp.dot(h, w_k[...], preferred_element_type=F32)
        for c in range(0, kv_width, piece):
            kv_out[rows, c : c + piece] = rotate(
                headnorm(k[:, c : c + piece], k_gain[:, :piece]), cos, sin
            ).astype(BF16)
        kv_out[rows, kv_width:] = jnp.dot(h, w_v[...], preferred_element_type=F32).astype(BF16)
        q = jnp.dot(h, w_q[...], preferred_element_type=F32)
        for c in range(0, q_width, 128):
            y = rotate(headnorm(q[:, c : c + 128], q_gain[...]), cos, sin).astype(BF16)
            y = y.astype(F32) * CHANNEL_SPAN ** (-0.5)
            lane = lax.broadcasted_iota(jnp.int32, y.shape, 1)
            for j in range(2):
                head = c // CHANNEL_SPAN + j
                place = head // group
                moved = y if place % 2 == j else pltpu.roll(y, 64, 1)
                base = place // 2 * 128
                inside = lane // CHANNEL_SPAN == place % 2
                blank = jnp.where(inside, moved, 0.0).astype(BF16)
                for b in range(0, kv_width, piece):
                    q_out[head, rows, b : b + piece] = (
                        blank[:, :piece] if b == base else jnp.zeros((own_rows, piece), BF16)
                    )
        return carry

    lax.fori_loop(0, n_tp, tile, 0)


def attend_kernel(
    n_sp, n_tp, tile_rows, offset, q, ctx, kv, latent, mods, w_out_hbm, out,
    ctx_all, kv_all, peak, total, acc, attended, received, w_out,
    kv_send, kv_recv, ctx_send, ctx_recv, at_send, at_recv, own_sem, w_sem,
):
    sp, tp = lax.axis_index("sp"), lax.axis_index("tp")
    tok, width2 = kv.shape
    width = width2 // 2
    kv_heads = width // CHANNEL_SPAN
    q_heads = q.shape[0]
    group = q_heads // kv_heads
    own_rows = tok // n_tp
    q_width = q_heads * CHANNEL_SPAN
    fetch = pltpu.make_async_copy(w_out_hbm, w_out, w_sem)
    fetch.start()
    greet(n_sp, n_tp)

    def kv_copy(d):
        return pltpu.make_async_remote_copy(
            src_ref=kv, dst_ref=kv_all.at[sp], send_sem=kv_send.at[d - 1],
            recv_sem=kv_recv.at[d - 1], device_id=(lax.rem(sp + d, n_sp), tp), device_id_type=MESH,
        )

    def ctx_copy(d):
        return pltpu.make_async_remote_copy(
            src_ref=ctx, dst_ref=ctx_all.at[sp], send_sem=ctx_send.at[d - 1],
            recv_sem=ctx_recv.at[d - 1], device_id=(lax.rem(sp + d, n_sp), tp), device_id_type=MESH,
        )

    def send(d, carry):
        kv_copy(d).start()
        ctx_copy(d).start()
        return carry

    lax.fori_loop(1, n_sp, send, 0)
    own = pltpu.make_async_copy(ctx, ctx_all.at[sp], own_sem)
    own.start()
    tiles = tok // tile_rows

    def update(keys, values, shift, first):
        def step(i, carry):
            head, r = i // tiles, lax.rem(i, tiles)
            rows = pl.ds(pl.multiple_of(r * tile_rows, tile_rows), tile_rows)
            s = lax.dot_general(
                q[head, rows, :], keys(), (((1,), (1,)), ((), ())), preferred_element_type=F32
            )
            if shift:
                s = s + shift
            top = jnp.max(s, axis=-1, keepdims=True)
            if not first:
                old = peak[head, rows, 0:1]
                top = jnp.maximum(top, old)
                shrink = jnp.exp(old - top)
            e = jnp.exp(s - top)
            row_sum = jnp.sum(e, axis=-1, keepdims=True)
            w = jnp.dot(e.astype(BF16), values(), preferred_element_type=F32)
            if not first:
                row_sum = row_sum + total[head, rows, 0:1] * shrink
                w = w + acc[head, rows, :] * shrink
            peak[head, rows, :] = jnp.broadcast_to(top, (tile_rows, 128))
            total[head, rows, :] = jnp.broadcast_to(row_sum, (tile_rows, 128))
            acc[head, rows, :] = w
            return carry

        lax.fori_loop(0, q_heads * tiles, step, 0)

    update(lambda: kv[:, :width], lambda: kv[:, width:], 0.0, True)

    def block(d, carry):
        kv_copy(d).wait_recv()
        src = lax.rem(sp + n_sp - d, n_sp)
        update(lambda: kv_all[src, :, :width], lambda: kv_all[src, :, width:], 0.0, False)
        return carry

    lax.fori_loop(1, n_sp, block, 0)
    own.wait()

    def ctx_wait(d, carry):
        ctx_copy(d).wait()
        kv_copy(d).wait_send()
        return carry

    lax.fori_loop(1, n_sp, ctx_wait, 0)
    ctx_count = n_sp * ctx.shape[0]
    update(
        lambda: ctx_all[:, :, :width].reshape(ctx_count, width),
        lambda: ctx_all[:, :, width:].reshape(ctx_count, width),
        offset,
        False,
    )
    for t in range(n_tp):
        rows = slice(t * own_rows, (t + 1) * own_rows)
        for h in range(q_heads):
            g = h // group
            a = acc[h, rows, :] / total[h, rows, 0:1]
            attended[t, :, h * CHANNEL_SPAN : (h + 1) * CHANNEL_SPAN] = a[
                :, g * CHANNEL_SPAN : (g + 1) * CHANNEL_SPAN
            ].astype(BF16)
    copies = []
    for d in range(1, n_tp):
        peer = lax.rem(tp + d, n_tp)
        c = pltpu.make_async_remote_copy(
            src_ref=attended.at[peer], dst_ref=received.at[tp], send_sem=at_send.at[d - 1],
            recv_sem=at_recv.at[d - 1], device_id=(sp, peer), device_id_type=MESH,
        )
        c.start()
        copies.append(c)
    received[tp] = attended[tp]
    fetch.wait()
    for c in copies:
        c.wait()
    span = mods.shape[2]
    for t in range(n_tp):
        cols = slice(t * span, (t + 1) * span)
        branch = jnp.zeros((own_rows, span), F32)
        for s in range(n_tp):
            branch = branch + jnp.dot(
                received[s],
                w_out[s * q_width : (s + 1) * q_width, cols],
                preferred_element_type=F32,
            )
        out[:, cols] = (latent[:, cols].astype(F32) + mods[t, 4:5, :] * branch).astype(BF16)


def on_device(
    latent, context, condition, context_condition, norm_gain, shift_weight, scale_weight,
    gate_weight, query_weight, key_weight, value_weight, query_gain, key_gain, output_weight,
):
    n_sp, n_tp = lax.axis_size("sp"), lax.axis_size("tp")
    seq_index = lax.axis_index("sp")
    row_slab, columns = shift_weight.shape
    own_rows, model = latent.shape
    ctx_rows = context.shape[0]
    tok = own_rows * n_tp
    q_width, kv_width = query_weight.shape[1], key_weight.shape[1]
    q_heads = q_width // CHANNEL_SPAN
    conditions = jnp.stack([condition, context_condition])
    act = jax.nn.silu(
        lax.dynamic_slice_in_dim(conditions, seq_index * row_slab, row_slab, 1)
    ).astype(BF16)
    act = jnp.pad(act, ((0, 14), (0, 0)))
    dma = pltpu.SemaphoreType.DMA
    lat_all, mods = pl.pallas_call(
        functools.partial(gather_kernel, n_sp, n_tp),
        out_shape=(
            jax.ShapeDtypeStruct((n_tp, own_rows, model), BF16),
            jax.ShapeDtypeStruct((n_tp, 8, columns), F32),
        ),
        in_specs=[VMEM] * 5,
        out_specs=(VMEM, VMEM),
        scratch_shapes=[
            pltpu.VMEM((8, columns), F32),
            pltpu.VMEM((n_sp, 8, columns), F32),
            dma((n_tp - 1,)), dma((n_tp - 1,)), dma((n_sp - 1,)), dma((n_sp - 1,)),
            dma((n_tp - 1,)), dma((n_tp - 1,)), dma,
        ],
        compiler_params=pltpu.CompilerParams(
            collective_id=0, has_side_effects=True, vmem_limit_bytes=30 << 20
        ),
        name="gather_rows",
    )(latent, act, shift_weight, scale_weight, gate_weight)

    quarter = CHANNEL_SPAN // 4
    places = seq_index * tok + jnp.arange(tok, dtype=jnp.int32)
    lane = jnp.arange(128, dtype=jnp.int32) % CHANNEL_SPAN
    inverse = rope_base ** (-(lane % quarter).astype(F32) / quarter)
    coord = jnp.where(
        lane[None, :] < 2 * quarter, (places // GRID_W)[:, None], (places % GRID_W)[:, None]
    ).astype(F32)
    angles = coord * inverse
    cosine = jnp.cos(angles)
    sine = jnp.where(lane % (2 * quarter) < quarter, -1.0, 1.0) * jnp.sin(angles)
    q, ctx, kv = pl.pallas_call(
        functools.partial(project_kernel, n_tp),
        out_shape=(
            jax.ShapeDtypeStruct((q_heads, tok, kv_width), BF16),
            jax.ShapeDtypeStruct((ctx_rows, 2 * kv_width), BF16),
            jax.ShapeDtypeStruct((tok, 2 * kv_width), BF16),
        ),
        in_specs=[VMEM] * 11,
        out_specs=(VMEM, VMEM, VMEM),
        scratch_shapes=[pltpu.VMEM((max(own_rows, ctx_rows), model), BF16)],
        compiler_params=pltpu.CompilerParams(vmem_limit_bytes=40 << 20),
        name="project",
    )(
        lat_all, context, mods, norm_gain[None], query_weight, key_weight, value_weight,
        jnp.tile(query_gain, 2)[None], jnp.tile(key_gain, 2)[None], cosine, sine,
    )
    offset = math.log(tok / (2.0 * ctx_rows))
    tile_rows = math.gcd(tok, 256)
    return pl.pallas_call(
        functools.partial(attend_kernel, n_sp, n_tp, tile_rows, offset),
        out_shape=jax.ShapeDtypeStruct(latent.shape, BF16),
        in_specs=[VMEM] * 5 + [pl.BlockSpec(memory_space=pl.ANY)],
        out_specs=VMEM,
        scratch_shapes=[
            pltpu.VMEM((n_sp, ctx_rows, 2 * kv_width), BF16),
            pltpu.VMEM((n_sp, tok, 2 * kv_width), BF16),
            pltpu.VMEM((q_heads, tok, 128), F32),
            pltpu.VMEM((q_heads, tok, 128), F32),
            pltpu.VMEM((q_heads, tok, kv_width), F32),
            pltpu.VMEM((n_tp, own_rows, q_width), BF16),
            pltpu.VMEM((n_tp, own_rows, q_width), BF16),
            pltpu.VMEM(output_weight.shape, BF16),
            dma((n_sp - 1,)), dma((n_sp - 1,)), dma((n_sp - 1,)), dma((n_sp - 1,)),
            dma((n_tp - 1,)), dma((n_tp - 1,)), dma, dma,
        ],
        compiler_params=pltpu.CompilerParams(
            collective_id=1, has_side_effects=True, vmem_limit_bytes=56 << 20
        ),
        name="attend",
    )(q, ctx, kv, latent, mods, output_weight)


def solution(mesh):
    in_specs = (
        P(("sp", "tp"), None), P("sp", None), P(), P(), P(),
        P("sp", "tp"), P("sp", "tp"), P("sp", "tp"),
        P(None, "tp"), P(None, "tp"), P(None, "tp"), P(), P(), P(),
    )
    return jax.shard_map(
        on_device, mesh=mesh, in_specs=in_specs, out_specs=P(("sp", "tp"), None), check_vma=False
    )
```

```python
import functools
import math

import jax
import jax.numpy as jnp
from jax import lax
from jax.experimental import pallas as pl
from jax.experimental.pallas import tpu as pltpu
from jax.sharding import PartitionSpec as P

CHANNEL_SPAN = 64
GRID_W = 64
TILE = 256
UNROLL = 2
MESH = pl.DeviceIdType.MESH
VMEM = pl.BlockSpec(memory_space=pltpu.VMEM)
F32 = jnp.float32
BF16 = jnp.bfloat16

epsilon = 1e-06
rope_base = 10000.0


def greet(n_sp, n_tp):
    sp, tp = lax.axis_index("sp"), lax.axis_index("tp")
    barrier = pltpu.get_barrier_semaphore()
    for d in range(1, n_sp):
        pl.semaphore_signal(
            barrier, inc=1, device_id=(lax.rem(sp + d, n_sp), tp), device_id_type=MESH
        )
    for d in range(1, n_tp):
        pl.semaphore_signal(
            barrier, inc=1, device_id=(sp, lax.rem(tp + d, n_tp)), device_id_type=MESH
        )
    pl.semaphore_wait(barrier, n_sp + n_tp - 2)


def gather_kernel(
    n_sp, n_tp, latent_hbm, act, w_shift_hbm, w_scale_hbm, w_gate_hbm, context_hbm, norm_gain,
    w_q_hbm, w_k_hbm, w_v_hbm, q_gain, k_gain, cosine, sine, q_out, kv_out, mods,
    lat_all, w_mod, context, w_q, w_k, w_v, hidden, part, parts,
    load, lat_send, lat_recv, fwd_send, sp_send, sp_recv, tp_send, tp_recv,
):
    sp, tp = lax.axis_index("sp"), lax.axis_index("tp")
    loads = [
        pltpu.make_async_copy(src, dst, load.at[i])
        for i, (src, dst) in enumerate(
            (
                (w_shift_hbm, w_mod.at[0]), (w_scale_hbm, w_mod.at[1]), (w_gate_hbm, w_mod.at[2]),
                (latent_hbm, lat_all.at[tp]), (context_hbm, context),
                (w_k_hbm, w_k), (w_v_hbm, w_v), (w_q_hbm, w_q),
            )
        )
    ]
    for c in loads:
        c.start()
    greet(n_sp, n_tp)
    core = lax.rem(tp, 2)
    twin = tp + 1 - 2 * core
    chips = n_tp // 2

    def row_copy(src, send_sem, peer):
        return pltpu.make_async_remote_copy(
            src_ref=lat_all.at[src], dst_ref=lat_all.at[src], send_sem=send_sem,
            recv_sem=lat_recv.at[src], device_id=(sp, peer), device_id_type=MESH,
        )

    part[...] = jnp.zeros_like(part)
    for i in range(3):
        loads[i].wait()
        part[2 * i : 2 * i + 2, :] = jnp.dot(act[...], w_mod[i], preferred_element_type=F32)[0:2]
    sp_copies = []
    for d in range(1, n_sp):
        c = pltpu.make_async_remote_copy(
            src_ref=part, dst_ref=parts.at[sp], send_sem=sp_send.at[d - 1],
            recv_sem=sp_recv.at[d - 1], device_id=(lax.rem(sp + d, n_sp), tp), device_id_type=MESH,
        )
        c.start()
        sp_copies.append(c)
    parts[sp] = part[...]
    loads[3].wait()
    sends = []
    for d in range(1, chips):
        sends.append(row_copy(tp, lat_send.at[d], lax.rem(tp + 2 * d, n_tp)))
    sends.append(row_copy(tp, lat_send.at[0], twin))
    for c in sends:
        c.start()
    for c in sp_copies:
        c.wait()
    total = parts[0]
    for j in range(1, n_sp):
        total = total + parts[j]
    part[...] = total
    mods[tp] = total
    tp_copies = []
    for d in range(1, n_tp):
        c = pltpu.make_async_remote_copy(
            src_ref=part, dst_ref=mods.at[tp], send_sem=tp_send.at[d - 1],
            recv_sem=tp_recv.at[d - 1], device_id=(sp, lax.rem(tp + d, n_tp)), device_id_type=MESH,
        )
        c.start()
        tp_copies.append(c)
    for c in loads[4:]:
        c.wait()
    for c in tp_copies:
        c.wait()
    context_step, tile = project(
        n_tp, lat_all, context, mods, norm_gain, w_q, w_k, w_v, q_gain, k_gain, cosine, sine,
        q_out, kv_out, hidden,
    )
    context_step()
    tile(tp)
    forwards = []
    for d in range(1, chips):
        src = lax.rem(tp - 2 * d + n_tp, n_tp)
        row_copy(src, lat_send.at[0], twin).wait_recv()
        c = row_copy(src, fwd_send.at[d - 1], twin)
        c.start()
        forwards.append(c)
    row_copy(twin, lat_send.at[0], twin).wait_recv()
    tile(twin)
    for d in range(1, chips):
        tile(lax.rem(tp - 2 * d + n_tp, n_tp))
    for d in range(1, chips):
        src = lax.rem(twin - 2 * d + n_tp, n_tp)
        row_copy(src, lat_send.at[0], twin).wait_recv()
        tile(src)
    for c in sends + forwards:
        c.wait_send()


def project(
    n_tp, lat_all, context, mods, norm_gain, w_q, w_k, w_v, q_gain, k_gain, cosine, sine,
    q_out, kv_out, hidden,
):
    own_rows = lat_all.shape[1]
    ctx_rows = context.shape[0]
    q_width = w_q.shape[1]
    kv_width = w_k.shape[1]
    kv_heads = kv_width // CHANNEL_SPAN
    q_heads = q_width // CHANNEL_SPAN
    group = q_heads // kv_heads
    span = mods.shape[2]

    def modulate(read, rows, row):
        total = jnp.zeros((rows, 1), F32)
        for t in range(n_tp):
            x = read(t).astype(F32)
            total = total + jnp.sum(x * x, axis=-1, keepdims=True)
        inv = lax.rsqrt(total / (n_tp * span) + epsilon)
        for t in range(n_tp):
            cols = slice(t * span, (t + 1) * span)
            x = read(t).astype(F32)
            y = x * inv * norm_gain[:, cols] * (1.0 + mods[t, 2 + row : 3 + row, :]) + mods[
                t, row : row + 1, :
            ]
            hidden[0:rows, cols] = y.astype(BF16)

    def headnorm(x, gain):
        width = x.shape[1]
        head = lax.broadcasted_iota(jnp.int32, x.shape, 1) // CHANNEL_SPAN
        sq = x * x
        scale = jnp.zeros_like(x)
        for h in range(width // CHANNEL_SPAN):
            s = jnp.sum(jnp.where(head == h, sq, 0.0), axis=-1, keepdims=True)
            scale = jnp.where(head == h, lax.rsqrt(s / CHANNEL_SPAN + epsilon), scale)
        return x * scale * gain

    def rotate(x, cos, sin):
        width = x.shape[1]
        full = x if width == 128 else jnp.concatenate([x, x], axis=1)
        lane = lax.broadcasted_iota(jnp.int32, full.shape, 1)
        other = jnp.where(lane % 32 < 16, pltpu.roll(full, 112, 1), pltpu.roll(full, 16, 1))
        return (full * cos + other * sin)[:, :width]

    piece = min(128, kv_width)

    def context_step():
        modulate(lambda t: context[:, t * span : (t + 1) * span], ctx_rows, 1)
        h = hidden[0:ctx_rows, :]
        k = jnp.dot(h, w_k[...], preferred_element_type=F32)
        for c in range(0, kv_width, piece):
            kv_out[0:ctx_rows, c : c + piece] = headnorm(
                k[:, c : c + piece], k_gain[:, :piece]
            ).astype(BF16)
        kv_out[0:ctx_rows, kv_width:] = jnp.dot(h, w_v[...], preferred_element_type=F32).astype(
            BF16
        )

    def tile(i):
        modulate(lambda t: lat_all[i, :, t * span : (t + 1) * span], own_rows, 0)
        h = hidden[0:own_rows, :]
        rows = pl.ds(pl.multiple_of(i * own_rows, own_rows), own_rows)
        cos, sin = cosine[rows, :], sine[rows, :]
        low = pl.ds(pl.multiple_of(ctx_rows + i * own_rows, 16), own_rows)
        k = jnp.dot(h, w_k[...], preferred_element_type=F32)
        for c in range(0, kv_width, piece):
            kv_out[low, c : c + piece] = rotate(
                headnorm(k[:, c : c + piece], k_gain[:, :piece]), cos, sin
            ).astype(BF16)
        kv_out[low, kv_width:] = jnp.dot(h, w_v[...], preferred_element_type=F32).astype(BF16)
        q = jnp.dot(h, w_q[...], preferred_element_type=F32)
        for c in range(0, q_width, 128):
            y = rotate(headnorm(q[:, c : c + 128], q_gain[...]), cos, sin).astype(BF16)
            y = y.astype(F32) * CHANNEL_SPAN ** (-0.5)
            lane = lax.broadcasted_iota(jnp.int32, y.shape, 1)
            for j in range(2):
                head = c // CHANNEL_SPAN + j
                place = head // group
                moved = y if place % 2 == j else pltpu.roll(y, 64, 1)
                base = place // 2 * 128
                inside = lane // CHANNEL_SPAN == place % 2
                blank = jnp.where(inside, moved, 0.0).astype(BF16)
                for b in range(0, kv_width, piece):
                    q_out[head, rows, b : b + piece] = (
                        blank[:, :piece] if b == base else jnp.zeros((own_rows, piece), BF16)
                    )

    return context_step, tile


def attend_kernel(
    n_sp, n_tp, lows, tile_rows, unroll, ctx_rows, offset, q, kv, mods, latent_hbm, w_out_hbm, out,
    kv_all, peak, total, acc, attended, received, latent, w_out,
    lo_send, hi_send, fwd_send, kv_recv, at_send, at_recv, own_sem, lat_sem, w_sem,
):
    sp, tp = lax.axis_index("sp"), lax.axis_index("tp")
    tok, width2 = q.shape[1], kv.shape[1]
    width = width2 // 2
    kv_heads = width // CHANNEL_SPAN
    q_heads = q.shape[0]
    group = q_heads // kv_heads
    own_rows = tok // n_tp
    q_width = q_heads * CHANNEL_SPAN
    fetch = pltpu.make_async_copy(w_out_hbm, w_out, w_sem)
    fetch_latent = pltpu.make_async_copy(latent_hbm, latent, lat_sem)
    greet(n_sp, n_tp)
    highs = n_sp // lows
    low, high = lax.rem(sp, lows), sp // lows

    def copy(src, slot, send_sem, peer):
        return pltpu.make_async_remote_copy(
            src_ref=slot, dst_ref=kv_all.at[src], send_sem=send_sem,
            recv_sem=kv_recv.at[src], device_id=(peer, tp), device_id_type=MESH,
        )

    def low_peer(d):
        return high * lows + lax.rem(low + d, lows)

    def high_peer(d):
        return lax.rem(high + d, highs) * lows + low

    sends = [copy(sp, kv, lo_send.at[d - 1], low_peer(d)) for d in range(1, lows)]
    sends += [copy(sp, kv, hi_send.at[d - 1], high_peer(d)) for d in range(1, highs)]
    for c in sends:
        c.start()
    own = pltpu.make_async_copy(kv, kv_all.at[sp], own_sem)
    own.start()
    fetch.start()
    fetch_latent.start()
    tiles = tok // tile_rows

    def update(keys, values, shift, first):
        def step(i, carry):
            head, r = i // tiles, lax.rem(i, tiles)
            rows = pl.ds(pl.multiple_of(r * tile_rows, tile_rows), tile_rows)
            s = lax.dot_general(
                q[head, rows, :], keys(), (((1,), (1,)), ((), ())), preferred_element_type=F32
            )
            if shift:
                s = s + shift
            top = jnp.max(s, axis=-1, keepdims=True)
            if not first:
                old = peak[head, rows, 0:1]
                top = jnp.maximum(top, old)
                shrink = jnp.exp(old - top)
            e = jnp.exp(s - top)
            row_sum = jnp.sum(e, axis=-1, keepdims=True)
            w = jnp.dot(e.astype(BF16), values(), preferred_element_type=F32)
            if not first:
                row_sum = row_sum + total[head, rows, 0:1] * shrink
                w = w + acc[head, rows, :] * shrink
            peak[head, rows, :] = jnp.broadcast_to(top, (tile_rows, 128))
            total[head, rows, :] = jnp.broadcast_to(row_sum, (tile_rows, 128))
            acc[head, rows, :] = w
            return carry

        lax.fori_loop(0, q_heads * tiles, step, 0, unroll=unroll)

    def attend(src):
        update(
            lambda: kv_all[src, ctx_rows:, :width], lambda: kv_all[src, ctx_rows:, width:],
            0.0, False,
        )

    def arrive(src):
        copy(src, kv, lo_send.at[0], low_peer(0)).wait_recv()

    update(lambda: kv[ctx_rows:, :width], lambda: kv[ctx_rows:, width:], 0.0, True)

    def near(d, carry):
        src = high * lows + lax.rem(low - d + lows, lows)
        arrive(src)
        attend(src)
        return carry

    lax.fori_loop(1, lows, near, 0)

    def column(d, carry):
        row = lax.rem(high - d + highs, highs) * lows
        src = row + low
        arrive(src)

        def pass_on(e, inner):
            copy(
                src, kv_all.at[src], fwd_send.at[(d - 1) * (lows - 1) + e - 1], low_peer(e)
            ).start()
            return inner

        lax.fori_loop(1, lows, pass_on, 0)
        attend(src)
        return carry

    lax.fori_loop(1, highs, column, 0)

    def rest(k, carry):
        d, e = k // (lows - 1) + 1, lax.rem(k, lows - 1) + 1
        src = lax.rem(high - d + highs, highs) * lows + lax.rem(low - e + lows, lows)
        arrive(src)
        attend(src)
        return carry

    lax.fori_loop(0, (highs - 1) * (lows - 1), rest, 0)
    own.wait()
    ctx_count = n_sp * ctx_rows
    update(
        lambda: kv_all[:, :ctx_rows, :width].reshape(ctx_count, width),
        lambda: kv_all[:, :ctx_rows, width:].reshape(ctx_count, width),
        offset,
        False,
    )
    for c in sends:
        c.wait_send()

    def sent(k, carry):
        copy(sp, kv, fwd_send.at[k], low_peer(1)).wait_send()
        return carry

    lax.fori_loop(0, (highs - 1) * (lows - 1), sent, 0)
    for t in range(n_tp):
        rows = slice(t * own_rows, (t + 1) * own_rows)
        for h in range(q_heads):
            g = h // group
            a = acc[h, rows, :] / total[h, rows, 0:1]
            attended[t, :, h * CHANNEL_SPAN : (h + 1) * CHANNEL_SPAN] = a[
                :, g * CHANNEL_SPAN : (g + 1) * CHANNEL_SPAN
            ].astype(BF16)
    copies = []
    for d in range(1, n_tp):
        peer = lax.rem(tp + d, n_tp)
        c = pltpu.make_async_remote_copy(
            src_ref=attended.at[peer], dst_ref=received.at[tp], send_sem=at_send.at[d - 1],
            recv_sem=at_recv.at[d - 1], device_id=(sp, peer), device_id_type=MESH,
        )
        c.start()
        copies.append(c)
    received[tp] = attended[tp]
    fetch.wait()
    fetch_latent.wait()
    for c in copies:
        c.wait()
    span = mods.shape[2]
    for t in range(n_tp):
        cols = slice(t * span, (t + 1) * span)
        branch = jnp.zeros((own_rows, span), F32)
        for s in range(n_tp):
            branch = branch + jnp.dot(
                received[s],
                w_out[s * q_width : (s + 1) * q_width, cols],
                preferred_element_type=F32,
            )
        out[:, cols] = (latent[:, cols].astype(F32) + mods[t, 4:5, :] * branch).astype(BF16)


def on_device(
    latent, context, condition, context_condition, norm_gain, shift_weight, scale_weight,
    gate_weight, query_weight, key_weight, value_weight, query_gain, key_gain, output_weight,
):
    n_sp, n_tp = lax.axis_size("sp"), lax.axis_size("tp")
    seq_index = lax.axis_index("sp")
    row_slab, columns = shift_weight.shape
    own_rows, model = latent.shape
    ctx_rows = context.shape[0]
    tok = own_rows * n_tp
    q_width, kv_width = query_weight.shape[1], key_weight.shape[1]
    q_heads = q_width // CHANNEL_SPAN
    conditions = jnp.stack([condition, context_condition])
    act = jax.nn.silu(
        lax.dynamic_slice_in_dim(conditions, seq_index * row_slab, row_slab, 1)
    ).astype(BF16)
    act = jnp.pad(act, ((0, 14), (0, 0)))
    dma = pltpu.SemaphoreType.DMA
    quarter = CHANNEL_SPAN // 4
    places = seq_index * tok + jnp.arange(tok, dtype=jnp.int32)
    lane = jnp.arange(128, dtype=jnp.int32) % CHANNEL_SPAN
    inverse = rope_base ** (-(lane % quarter).astype(F32) / quarter)
    coord = jnp.where(
        lane[None, :] < 2 * quarter, (places // GRID_W)[:, None], (places % GRID_W)[:, None]
    ).astype(F32)
    angles = coord * inverse
    cosine = jnp.cos(angles)
    sine = jnp.where(lane % (2 * quarter) < quarter, -1.0, 1.0) * jnp.sin(angles)
    anywhere = pl.BlockSpec(memory_space=pl.ANY)
    q, kv, mods = pl.pallas_call(
        functools.partial(gather_kernel, n_sp, n_tp),
        out_shape=(
            jax.ShapeDtypeStruct((q_heads, tok, kv_width), BF16),
            jax.ShapeDtypeStruct((ctx_rows + tok, 2 * kv_width), BF16),
            jax.ShapeDtypeStruct((n_tp, 8, columns), F32),
        ),
        in_specs=[anywhere, VMEM] + [anywhere] * 4 + [VMEM] + [anywhere] * 3 + [VMEM] * 4,
        out_specs=(VMEM, VMEM, VMEM),
        scratch_shapes=[
            pltpu.VMEM((n_tp, own_rows, model), BF16),
            pltpu.VMEM((3, row_slab, columns), BF16),
            pltpu.VMEM(context.shape, BF16),
            pltpu.VMEM(query_weight.shape, BF16),
            pltpu.VMEM(key_weight.shape, BF16),
            pltpu.VMEM(value_weight.shape, BF16),
            pltpu.VMEM((max(own_rows, ctx_rows), model), BF16),
            pltpu.VMEM((8, columns), F32),
            pltpu.VMEM((n_sp, 8, columns), F32),
            dma((8,)), dma((n_tp // 2,)), dma((n_tp,)), dma((max(n_tp // 2 - 1, 1),)),
            dma((n_sp - 1,)), dma((n_sp - 1,)), dma((n_tp - 1,)), dma((n_tp - 1,)),
        ],
        compiler_params=pltpu.CompilerParams(
            collective_id=0, has_side_effects=True, vmem_limit_bytes=56 << 20
        ),
        name="gather_project",
    )(
        latent, act, shift_weight, scale_weight, gate_weight, context, norm_gain[None],
        query_weight, key_weight, value_weight,
        jnp.tile(query_gain, 2)[None], jnp.tile(key_gain, 2)[None], cosine, sine,
    )
    offset = math.log(tok / (2.0 * ctx_rows))
    tile_rows = math.gcd(tok, TILE)
    lows = 2 ** (int(math.log2(n_sp)) // 2)
    return pl.pallas_call(
        functools.partial(
            attend_kernel, n_sp, n_tp, lows, tile_rows, UNROLL, ctx_rows, offset
        ),
        out_shape=jax.ShapeDtypeStruct(latent.shape, BF16),
        in_specs=[VMEM] * 3 + [anywhere] * 2,
        out_specs=VMEM,
        scratch_shapes=[
            pltpu.VMEM((n_sp, ctx_rows + tok, 2 * kv_width), BF16),
            pltpu.VMEM((q_heads, tok, 128), F32),
            pltpu.VMEM((q_heads, tok, 128), F32),
            pltpu.VMEM((q_heads, tok, kv_width), F32),
            pltpu.VMEM((n_tp, own_rows, q_width), BF16),
            pltpu.VMEM((n_tp, own_rows, q_width), BF16),
            pltpu.VMEM(latent.shape, BF16),
            pltpu.VMEM(output_weight.shape, BF16),
            dma((lows - 1,)), dma((n_sp // lows - 1,)),
            dma(((n_sp // lows - 1) * (lows - 1),)), dma((n_sp,)),
            dma((n_tp - 1,)), dma((n_tp - 1,)), dma, dma, dma,
        ],
        compiler_params=pltpu.CompilerParams(
            collective_id=1, has_side_effects=True, vmem_limit_bytes=56 << 20
        ),
        name="attend",
    )(q, kv, mods, latent, output_weight)


def solution(mesh):
    in_specs = (
        P(("sp", "tp"), None), P("sp", None), P(), P(), P(),
        P("sp", "tp"), P("sp", "tp"), P("sp", "tp"),
        P(None, "tp"), P(None, "tp"), P(None, "tp"), P(), P(), P(),
    )
    return jax.shard_map(
        on_device, mesh=mesh, in_specs=in_specs, out_specs=P(("sp", "tp"), None), check_vma=False
    )
```

```python
import functools
import math

import jax
import jax.numpy as jnp
from jax import lax
from jax.experimental import pallas as pl
from jax.experimental.pallas import tpu as pltpu
from jax.sharding import PartitionSpec as P

CHANNEL_SPAN = 64
GRID_W = 64
TILE = 512
UNROLL = 4
MESH = pl.DeviceIdType.MESH
VMEM = pl.BlockSpec(memory_space=pltpu.VMEM)
F32 = jnp.float32
BF16 = jnp.bfloat16

epsilon = 1e-06
rope_base = 10000.0


def greet(n_sp, n_tp):
    sp, tp = lax.axis_index("sp"), lax.axis_index("tp")
    barrier = pltpu.get_barrier_semaphore()
    for d in range(1, n_sp):
        pl.semaphore_signal(
            barrier, inc=1, device_id=(lax.rem(sp + d, n_sp), tp), device_id_type=MESH
        )
    for d in range(1, n_tp):
        pl.semaphore_signal(
            barrier, inc=1, device_id=(sp, lax.rem(tp + d, n_tp)), device_id_type=MESH
        )
    pl.semaphore_wait(barrier, n_sp + n_tp - 2)


def gather_kernel(
    n_sp, n_tp, latent_hbm, act, w_shift_hbm, w_scale_hbm, w_gate_hbm, context_hbm, norm_gain,
    w_q_hbm, w_k_hbm, w_v_hbm, q_gain, k_gain, cosine, sine, q_out, kv_out, mods,
    lat_all, w_mod, context, w_q, w_k, w_v, hidden, part, parts,
    load, lat_send, lat_recv, fwd_send, sp_send, sp_recv, tp_send, tp_recv,
):
    sp, tp = lax.axis_index("sp"), lax.axis_index("tp")
    loads = [
        pltpu.make_async_copy(src, dst, load.at[i])
        for i, (src, dst) in enumerate(
            (
                (w_shift_hbm, w_mod.at[0]), (w_scale_hbm, w_mod.at[1]), (w_gate_hbm, w_mod.at[2]),
                (latent_hbm, lat_all.at[tp]), (context_hbm, context),
                (w_k_hbm, w_k), (w_v_hbm, w_v), (w_q_hbm, w_q),
            )
        )
    ]
    loads[3].start()
    for i, c in enumerate(loads):
        if i != 3:
            c.start()
    greet(n_sp, n_tp)
    core = lax.rem(tp, 2)
    twin = tp + 1 - 2 * core
    chips = n_tp // 2

    def row_copy(src, send_sem, peer):
        return pltpu.make_async_remote_copy(
            src_ref=lat_all.at[src], dst_ref=lat_all.at[src], send_sem=send_sem,
            recv_sem=lat_recv.at[src], device_id=(sp, peer), device_id_type=MESH,
        )

    loads[3].wait()
    sends = []
    for d in range(1, chips):
        sends.append(row_copy(tp, lat_send.at[d], lax.rem(tp + 2 * d, n_tp)))
    sends.append(row_copy(tp, lat_send.at[0], twin))
    for c in sends:
        c.start()
    part[...] = jnp.zeros_like(part)
    for i in range(3):
        loads[i].wait()
        part[2 * i : 2 * i + 2, :] = jnp.dot(act[...], w_mod[i], preferred_element_type=F32)
    sp_copies = []
    for d in range(1, n_sp):
        c = pltpu.make_async_remote_copy(
            src_ref=part, dst_ref=parts.at[sp], send_sem=sp_send.at[d - 1],
            recv_sem=sp_recv.at[d - 1], device_id=(lax.rem(sp + d, n_sp), tp), device_id_type=MESH,
        )
        c.start()
        sp_copies.append(c)
    parts[sp] = part[...]
    for c in sp_copies:
        c.wait()
    total = parts[0]
    for j in range(1, n_sp):
        total = total + parts[j]
    part[...] = total
    mods[tp] = total
    tp_copies = []
    for d in range(1, n_tp):
        c = pltpu.make_async_remote_copy(
            src_ref=part, dst_ref=mods.at[tp], send_sem=tp_send.at[d - 1],
            recv_sem=tp_recv.at[d - 1], device_id=(sp, lax.rem(tp + d, n_tp)), device_id_type=MESH,
        )
        c.start()
        tp_copies.append(c)
    for c in loads[4:]:
        c.wait()
    for c in tp_copies:
        c.wait()
    context_step, tile = project(
        n_tp, lat_all, context, mods, norm_gain, w_q, w_k, w_v, q_gain, k_gain, cosine, sine,
        q_out, kv_out, hidden,
    )
    context_step()
    tile(tp)
    forwards = []
    for d in range(1, chips):
        src = lax.rem(tp - 2 * d + n_tp, n_tp)
        row_copy(src, lat_send.at[0], twin).wait_recv()
        c = row_copy(src, fwd_send.at[d - 1], twin)
        c.start()
        forwards.append(c)
    row_copy(twin, lat_send.at[0], twin).wait_recv()
    tile(twin)
    for d in range(1, chips):
        tile(lax.rem(tp - 2 * d + n_tp, n_tp))
    for d in range(1, chips):
        src = lax.rem(twin - 2 * d + n_tp, n_tp)
        row_copy(src, lat_send.at[0], twin).wait_recv()
        tile(src)
    for c in sends + forwards:
        c.wait_send()


def project(
    n_tp, lat_all, context, mods, norm_gain, w_q, w_k, w_v, q_gain, k_gain, cosine, sine,
    q_out, kv_out, hidden,
):
    own_rows = lat_all.shape[1]
    ctx_rows = context.shape[0]
    q_width = w_q.shape[1]
    kv_width = w_k.shape[1]
    kv_heads = kv_width // CHANNEL_SPAN
    q_heads = q_width // CHANNEL_SPAN
    group = q_heads // kv_heads
    span = mods.shape[2]

    def modulate(read, rows, row):
        total = jnp.zeros((rows, 1), F32)
        for t in range(n_tp):
            x = read(t).astype(F32)
            total = total + jnp.sum(x * x, axis=-1, keepdims=True)
        inv = lax.rsqrt(total / (n_tp * span) + epsilon)
        for t in range(n_tp):
            cols = slice(t * span, (t + 1) * span)
            x = read(t).astype(F32)
            y = x * inv * norm_gain[:, cols] * (1.0 + mods[t, 2 + row : 3 + row, :]) + mods[
                t, row : row + 1, :
            ]
            hidden[0:rows, cols] = y.astype(BF16)

    def headnorm(x, gain):
        width = x.shape[1]
        head = lax.broadcasted_iota(jnp.int32, x.shape, 1) // CHANNEL_SPAN
        sq = x * x
        scale = jnp.zeros_like(x)
        for h in range(width // CHANNEL_SPAN):
            s = jnp.sum(jnp.where(head == h, sq, 0.0), axis=-1, keepdims=True)
            scale = jnp.where(head == h, lax.rsqrt(s / CHANNEL_SPAN + epsilon), scale)
        return x * scale * gain

    def rotate(x, cos, sin):
        width = x.shape[1]
        full = x if width == 128 else jnp.concatenate([x, x], axis=1)
        lane = lax.broadcasted_iota(jnp.int32, full.shape, 1)
        other = jnp.where(lane % 32 < 16, pltpu.roll(full, 112, 1), pltpu.roll(full, 16, 1))
        return (full * cos + other * sin)[:, :width]

    piece = min(128, kv_width)
    q_pair = jnp.concatenate([q_gain[...], q_gain[...]], axis=1)
    k_pair = jnp.concatenate([k_gain[...], k_gain[...]], axis=1)

    def context_step():
        modulate(lambda t: context[:, t * span : (t + 1) * span], ctx_rows, 1)
        h = hidden[0:ctx_rows, :]
        k = jnp.dot(h, w_k[...], preferred_element_type=F32)
        for c in range(0, kv_width, piece):
            kv_out[0:ctx_rows, c : c + piece] = headnorm(
                k[:, c : c + piece], k_pair[:, :piece]
            ).astype(BF16)
        kv_out[0:ctx_rows, kv_width:] = jnp.dot(h, w_v[...], preferred_element_type=F32).astype(
            BF16
        )

    def tile(i):
        modulate(lambda t: lat_all[i, :, t * span : (t + 1) * span], own_rows, 0)
        h = hidden[0:own_rows, :]
        rows = pl.ds(pl.multiple_of(i * own_rows, own_rows), own_rows)
        cos, sin = cosine[rows, :], sine[rows, :]
        low = pl.ds(pl.multiple_of(ctx_rows + i * own_rows, 16), own_rows)
        k = jnp.dot(h, w_k[...], preferred_element_type=F32)
        for c in range(0, kv_width, piece):
            kv_out[low, c : c + piece] = rotate(
                headnorm(k[:, c : c + piece], k_pair[:, :piece]), cos, sin
            ).astype(BF16)
        kv_out[low, kv_width:] = jnp.dot(h, w_v[...], preferred_element_type=F32).astype(BF16)
        q = jnp.dot(h, w_q[...], preferred_element_type=F32)
        for c in range(0, q_width, 128):
            y = rotate(headnorm(q[:, c : c + 128], q_pair), cos, sin).astype(BF16)
            y = y.astype(F32) * CHANNEL_SPAN ** (-0.5)
            lane = lax.broadcasted_iota(jnp.int32, y.shape, 1)
            for j in range(2):
                head = c // CHANNEL_SPAN + j
                place = head // group
                moved = y if place % 2 == j else pltpu.roll(y, 64, 1)
                base = place // 2 * 128
                inside = lane // CHANNEL_SPAN == place % 2
                blank = jnp.where(inside, moved, 0.0).astype(BF16)
                for b in range(0, kv_width, piece):
                    q_out[head, rows, b : b + piece] = (
                        blank[:, :piece] if b == base else jnp.zeros((own_rows, piece), BF16)
                    )

    return context_step, tile


def attend_kernel(
    n_sp, n_tp, lows, tile_rows, unroll, ctx_rows, offset, q, kv, mods, latent_hbm, w_out_hbm, out,
    kv_all, peak, total, acc, attended, received, latent, w_out,
    lo_send, hi_send, fwd_send, kv_recv, at_send, at_recv, own_sem, lat_sem, w_sem,
):
    sp, tp = lax.axis_index("sp"), lax.axis_index("tp")
    tok, width2 = q.shape[1], kv.shape[1]
    width = width2 // 2
    kv_heads = width // CHANNEL_SPAN
    q_heads = q.shape[0]
    group = q_heads // kv_heads
    own_rows = tok // n_tp
    q_width = q_heads * CHANNEL_SPAN
    fetch = pltpu.make_async_copy(w_out_hbm, w_out, w_sem)
    fetch_latent = pltpu.make_async_copy(latent_hbm, latent, lat_sem)
    greet(n_sp, n_tp)
    highs = n_sp // lows
    low, high = lax.rem(sp, lows), sp // lows

    def copy(src, slot, send_sem, peer):
        return pltpu.make_async_remote_copy(
            src_ref=slot, dst_ref=kv_all.at[src], send_sem=send_sem,
            recv_sem=kv_recv.at[src], device_id=(peer, tp), device_id_type=MESH,
        )

    def low_peer(d):
        return high * lows + lax.rem(low + d, lows)

    def high_peer(d):
        return lax.rem(high + d, highs) * lows + low

    sends = [copy(sp, kv, lo_send.at[d - 1], low_peer(d)) for d in range(1, lows)]
    sends += [copy(sp, kv, hi_send.at[d - 1], high_peer(d)) for d in range(1, highs)]
    for c in sends:
        c.start()
    own = pltpu.make_async_copy(kv, kv_all.at[sp], own_sem)
    own.start()
    fetch.start()
    fetch_latent.start()
    tiles = tok // tile_rows

    def update(keys, values, shift, first):
        def step(i, carry):
            head, r = i // tiles, lax.rem(i, tiles)
            rows = pl.ds(pl.multiple_of(r * tile_rows, tile_rows), tile_rows)
            s = lax.dot_general(
                q[head, rows, :], keys(), (((1,), (1,)), ((), ())), preferred_element_type=F32
            )
            if shift:
                s = s + shift
            top = jnp.max(s, axis=-1, keepdims=True)
            if not first:
                old = peak[head, rows, 0:1]
                top = jnp.maximum(top, old)
                shrink = jnp.exp(old - top)
            e = jnp.exp(s - top)
            row_sum = e[:, 0:128]
            for c in range(128, e.shape[1], 128):
                row_sum = row_sum + e[:, c : c + 128]
            w = jnp.dot(e.astype(BF16), values(), preferred_element_type=F32)
            if not first:
                row_sum = row_sum + total[head, rows, :] * shrink
                w = w + acc[head, rows, :] * shrink
            peak[head, rows, :] = jnp.broadcast_to(top, (tile_rows, 128))
            total[head, rows, :] = row_sum
            acc[head, rows, :] = w
            return carry

        lax.fori_loop(0, q_heads * tiles, step, 0, unroll=unroll)

    def attend(src):
        update(
            lambda: kv_all[src, ctx_rows:, :width], lambda: kv_all[src, ctx_rows:, width:],
            0.0, False,
        )

    def arrive(src):
        copy(src, kv, lo_send.at[0], low_peer(0)).wait_recv()

    update(lambda: kv[ctx_rows:, :width], lambda: kv[ctx_rows:, width:], 0.0, True)

    def near(d, carry):
        src = high * lows + lax.rem(low - d + lows, lows)
        arrive(src)
        attend(src)
        return carry

    lax.fori_loop(1, lows, near, 0)

    def column(d, carry):
        row = lax.rem(high - d + highs, highs) * lows
        src = row + low
        arrive(src)

        def pass_on(e, inner):
            copy(
                src, kv_all.at[src], fwd_send.at[(d - 1) * (lows - 1) + e - 1], low_peer(e)
            ).start()
            return inner

        lax.fori_loop(1, lows, pass_on, 0)
        attend(src)
        return carry

    lax.fori_loop(1, highs, column, 0)

    def rest(k, carry):
        d, e = k // (lows - 1) + 1, lax.rem(k, lows - 1) + 1
        src = lax.rem(high - d + highs, highs) * lows + lax.rem(low - e + lows, lows)
        arrive(src)
        attend(src)
        return carry

    lax.fori_loop(0, (highs - 1) * (lows - 1), rest, 0)
    own.wait()
    ctx_count = n_sp * ctx_rows
    update(
        lambda: kv_all[:, :ctx_rows, :width].reshape(ctx_count, width),
        lambda: kv_all[:, :ctx_rows, width:].reshape(ctx_count, width),
        offset,
        False,
    )
    for c in sends:
        c.wait_send()

    def sent(k, carry):
        copy(sp, kv, fwd_send.at[k], low_peer(1)).wait_send()
        return carry

    lax.fori_loop(0, (highs - 1) * (lows - 1), sent, 0)
    for t in range(n_tp):
        rows = slice(t * own_rows, (t + 1) * own_rows)
        for h in range(q_heads):
            g = h // group
            a = acc[h, rows, :] / jnp.sum(total[h, rows, :], axis=-1, keepdims=True)
            attended[t, :, h * CHANNEL_SPAN : (h + 1) * CHANNEL_SPAN] = a[
                :, g * CHANNEL_SPAN : (g + 1) * CHANNEL_SPAN
            ].astype(BF16)
    copies = []
    for d in range(1, n_tp):
        peer = lax.rem(tp + d, n_tp)
        c = pltpu.make_async_remote_copy(
            src_ref=attended.at[peer], dst_ref=received.at[tp], send_sem=at_send.at[d - 1],
            recv_sem=at_recv.at[d - 1], device_id=(sp, peer), device_id_type=MESH,
        )
        c.start()
        copies.append(c)
    received[tp] = attended[tp]
    fetch.wait()
    fetch_latent.wait()
    for c in copies:
        c.wait()
    span = mods.shape[2]
    for t in range(n_tp):
        cols = slice(t * span, (t + 1) * span)
        branch = jnp.zeros((own_rows, span), F32)
        for s in range(n_tp):
            branch = branch + jnp.dot(
                received[s],
                w_out[s * q_width : (s + 1) * q_width, cols],
                preferred_element_type=F32,
            )
        out[:, cols] = (latent[:, cols].astype(F32) + mods[t, 4:5, :] * branch).astype(BF16)


def on_device(
    latent, context, condition, context_condition, norm_gain, shift_weight, scale_weight,
    gate_weight, query_weight, key_weight, value_weight, query_gain, key_gain, output_weight,
):
    n_sp, n_tp = lax.axis_size("sp"), lax.axis_size("tp")
    seq_index = lax.axis_index("sp")
    row_slab, columns = shift_weight.shape
    own_rows, model = latent.shape
    ctx_rows = context.shape[0]
    tok = own_rows * n_tp
    q_width, kv_width = query_weight.shape[1], key_weight.shape[1]
    q_heads = q_width // CHANNEL_SPAN
    conditions = jnp.stack([condition, context_condition])
    act = jax.nn.silu(
        lax.dynamic_slice_in_dim(conditions, seq_index * row_slab, row_slab, 1)
    ).astype(BF16)
    dma = pltpu.SemaphoreType.DMA
    quarter = CHANNEL_SPAN // 4
    places = seq_index * tok + jnp.arange(tok, dtype=jnp.int32)
    lane = jnp.arange(128, dtype=jnp.int32) % CHANNEL_SPAN
    inverse = rope_base ** (-(lane % quarter).astype(F32) / quarter)
    coord = jnp.where(
        lane[None, :] < 2 * quarter, (places // GRID_W)[:, None], (places % GRID_W)[:, None]
    ).astype(F32)
    angles = coord * inverse
    cosine = jnp.cos(angles)
    sine = jnp.where(lane % (2 * quarter) < quarter, -1.0, 1.0) * jnp.sin(angles)
    anywhere = pl.BlockSpec(memory_space=pl.ANY)
    q, kv, mods = pl.pallas_call(
        functools.partial(gather_kernel, n_sp, n_tp),
        out_shape=(
            jax.ShapeDtypeStruct((q_heads, tok, kv_width), BF16),
            jax.ShapeDtypeStruct((ctx_rows + tok, 2 * kv_width), BF16),
            jax.ShapeDtypeStruct((n_tp, 8, columns), F32),
        ),
        in_specs=[anywhere, VMEM] + [anywhere] * 4 + [VMEM] + [anywhere] * 3 + [VMEM] * 4,
        out_specs=(VMEM, VMEM, VMEM),
        scratch_shapes=[
            pltpu.VMEM((n_tp, own_rows, model), BF16),
            pltpu.VMEM((3, row_slab, columns), BF16),
            pltpu.VMEM(context.shape, BF16),
            pltpu.VMEM(query_weight.shape, BF16),
            pltpu.VMEM(key_weight.shape, BF16),
            pltpu.VMEM(value_weight.shape, BF16),
            pltpu.VMEM((max(own_rows, ctx_rows), model), BF16),
            pltpu.VMEM((8, columns), F32),
            pltpu.VMEM((n_sp, 8, columns), F32),
            dma((8,)), dma((n_tp // 2,)), dma((n_tp,)), dma((max(n_tp // 2 - 1, 1),)),
            dma((n_sp - 1,)), dma((n_sp - 1,)), dma((n_tp - 1,)), dma((n_tp - 1,)),
        ],
        compiler_params=pltpu.CompilerParams(
            collective_id=0, has_side_effects=True, vmem_limit_bytes=56 << 20
        ),
        name="gather_project",
    )(
        latent, act, shift_weight, scale_weight, gate_weight, context, norm_gain[None],
        query_weight, key_weight, value_weight,
        query_gain[None], key_gain[None], cosine, sine,
    )
    offset = math.log(tok / (2.0 * ctx_rows))
    tile_rows = math.gcd(tok, TILE)
    lows = 2 ** (int(math.log2(n_sp)) // 2)
    return pl.pallas_call(
        functools.partial(
            attend_kernel, n_sp, n_tp, lows, tile_rows, UNROLL, ctx_rows, offset
        ),
        out_shape=jax.ShapeDtypeStruct(latent.shape, BF16),
        in_specs=[VMEM] * 3 + [anywhere] * 2,
        out_specs=VMEM,
        scratch_shapes=[
            pltpu.VMEM((n_sp, ctx_rows + tok, 2 * kv_width), BF16),
            pltpu.VMEM((q_heads, tok, 128), F32),
            pltpu.VMEM((q_heads, tok, 128), F32),
            pltpu.VMEM((q_heads, tok, kv_width), F32),
            pltpu.VMEM((n_tp, own_rows, q_width), BF16),
            pltpu.VMEM((n_tp, own_rows, q_width), BF16),
            pltpu.VMEM(latent.shape, BF16),
            pltpu.VMEM(output_weight.shape, BF16),
            dma((lows - 1,)), dma((n_sp // lows - 1,)),
            dma(((n_sp // lows - 1) * (lows - 1),)), dma((n_sp,)),
            dma((n_tp - 1,)), dma((n_tp - 1,)), dma, dma, dma,
        ],
        compiler_params=pltpu.CompilerParams(
            collective_id=1, has_side_effects=True, vmem_limit_bytes=56 << 20
        ),
        name="attend",
    )(q, kv, mods, latent, output_weight)


def solution(mesh):
    in_specs = (
        P(("sp", "tp"), None), P("sp", None), P(), P(), P(),
        P("sp", "tp"), P("sp", "tp"), P("sp", "tp"),
        P(None, "tp"), P(None, "tp"), P(None, "tp"), P(), P(), P(),
    )
    return jax.shard_map(
        on_device, mesh=mesh, in_specs=in_specs, out_specs=P(("sp", "tp"), None), check_vma=False
    )
```

```python
import functools
import math

import jax
import jax.numpy as jnp
from jax import lax
from jax.experimental import pallas as pl
from jax.experimental.pallas import tpu as pltpu
from jax.sharding import PartitionSpec as P

CHANNEL_SPAN = 64
GRID_W = 64
TILE = 512
UNROLL = 4
MESH = pl.DeviceIdType.MESH
VMEM = pl.BlockSpec(memory_space=pltpu.VMEM)
F32 = jnp.float32
BF16 = jnp.bfloat16

epsilon = 1e-06
rope_base = 10000.0


def greet(n_sp, n_tp):
    sp, tp = lax.axis_index("sp"), lax.axis_index("tp")
    barrier = pltpu.get_barrier_semaphore()
    for d in range(1, n_sp):
        pl.semaphore_signal(
            barrier, inc=1, device_id=(lax.rem(sp + d, n_sp), tp), device_id_type=MESH
        )
    for d in range(1, n_tp):
        pl.semaphore_signal(
            barrier, inc=1, device_id=(sp, lax.rem(tp + d, n_tp)), device_id_type=MESH
        )
    pl.semaphore_wait(barrier, n_sp + n_tp - 2)


def gather_kernel(
    n_sp, n_tp, latent_hbm, act, w_shift_hbm, w_scale_hbm, w_gate_hbm, context_hbm, norm_gain,
    w_q_hbm, w_k_hbm, w_v_hbm, q_gain, k_gain, inverse, q_out, kv_out, mods,
    lat_all, w_mod, context, w_q, w_k, w_v, hidden, part, parts,
    cosine, sine, load, lat_send, lat_recv, fwd_send, sp_send, sp_recv, tp_send, tp_recv,
):
    sp, tp = lax.axis_index("sp"), lax.axis_index("tp")
    loads = [
        pltpu.make_async_copy(src, dst, load.at[i])
        for i, (src, dst) in enumerate(
            (
                (w_shift_hbm, w_mod.at[0]), (w_scale_hbm, w_mod.at[1]), (w_gate_hbm, w_mod.at[2]),
                (latent_hbm, lat_all.at[tp]), (context_hbm, context),
                (w_k_hbm, w_k), (w_v_hbm, w_v), (w_q_hbm, w_q),
            )
        )
    ]
    loads[3].start()
    for i, c in enumerate(loads):
        if i != 3:
            c.start()
    greet(n_sp, n_tp)
    core = lax.rem(tp, 2)
    twin = tp + 1 - 2 * core
    chips = n_tp // 2

    def row_copy(src, send_sem, peer):
        return pltpu.make_async_remote_copy(
            src_ref=lat_all.at[src], dst_ref=lat_all.at[src], send_sem=send_sem,
            recv_sem=lat_recv.at[src], device_id=(sp, peer), device_id_type=MESH,
        )

    loads[3].wait()
    sends = []
    for d in range(1, chips):
        sends.append(row_copy(tp, lat_send.at[d], lax.rem(tp + 2 * d, n_tp)))
    sends.append(row_copy(tp, lat_send.at[0], twin))
    for c in sends:
        c.start()
    part[...] = jnp.zeros_like(part)
    for i in range(3):
        loads[i].wait()
        part[2 * i : 2 * i + 2, :] = jnp.dot(act[...], w_mod[i], preferred_element_type=F32)
    sp_copies = []
    for d in range(1, n_sp):
        c = pltpu.make_async_remote_copy(
            src_ref=part, dst_ref=parts.at[sp], send_sem=sp_send.at[d - 1],
            recv_sem=sp_recv.at[d - 1], device_id=(lax.rem(sp + d, n_sp), tp), device_id_type=MESH,
        )
        c.start()
        sp_copies.append(c)
    parts[sp] = part[...]
    tok = cosine.shape[0]
    place = sp * tok + lax.broadcasted_iota(jnp.int32, (tok, 128), 0)
    lane = lax.broadcasted_iota(jnp.int32, (tok, 128), 1) % CHANNEL_SPAN
    coord = jnp.where(lane < CHANNEL_SPAN // 2, place // GRID_W, place % GRID_W)
    angles = coord.astype(F32) * inverse[...]
    cosine[...] = jnp.cos(angles)
    turn = jnp.sin(angles)
    sine[...] = jnp.where(lane % (CHANNEL_SPAN // 2) < CHANNEL_SPAN // 4, -turn, turn)
    for c in sp_copies:
        c.wait()
    total = parts[0]
    for j in range(1, n_sp):
        total = total + parts[j]
    part[...] = total
    mods[tp] = total
    tp_copies = []
    for d in range(1, n_tp):
        c = pltpu.make_async_remote_copy(
            src_ref=part, dst_ref=mods.at[tp], send_sem=tp_send.at[d - 1],
            recv_sem=tp_recv.at[d - 1], device_id=(sp, lax.rem(tp + d, n_tp)), device_id_type=MESH,
        )
        c.start()
        tp_copies.append(c)
    for c in loads[4:]:
        c.wait()
    for c in tp_copies:
        c.wait()
    context_step, tile = project(
        n_tp, lat_all, context, mods, norm_gain, w_q, w_k, w_v, q_gain, k_gain, cosine, sine,
        q_out, kv_out, hidden,
    )
    context_step()
    tile(tp)
    forwards = []
    for d in range(1, chips):
        src = lax.rem(tp - 2 * d + n_tp, n_tp)
        row_copy(src, lat_send.at[0], twin).wait_recv()
        c = row_copy(src, fwd_send.at[d - 1], twin)
        c.start()
        forwards.append(c)
    row_copy(twin, lat_send.at[0], twin).wait_recv()
    tile(twin)
    for d in range(1, chips):
        tile(lax.rem(tp - 2 * d + n_tp, n_tp))
    for d in range(1, chips):
        src = lax.rem(twin - 2 * d + n_tp, n_tp)
        row_copy(src, lat_send.at[0], twin).wait_recv()
        tile(src)
    for c in sends + forwards:
        c.wait_send()


def project(
    n_tp, lat_all, context, mods, norm_gain, w_q, w_k, w_v, q_gain, k_gain, cosine, sine,
    q_out, kv_out, hidden,
):
    own_rows = lat_all.shape[1]
    ctx_rows = context.shape[0]
    q_width = w_q.shape[1]
    kv_width = w_k.shape[1]
    kv_heads = kv_width // CHANNEL_SPAN
    q_heads = q_width // CHANNEL_SPAN
    group = q_heads // kv_heads
    span = mods.shape[2]

    def modulate(read, rows, row):
        total = jnp.zeros((rows, 1), F32)
        for t in range(n_tp):
            x = read(t).astype(F32)
            total = total + jnp.sum(x * x, axis=-1, keepdims=True)
        inv = lax.rsqrt(total / (n_tp * span) + epsilon)
        for t in range(n_tp):
            cols = slice(t * span, (t + 1) * span)
            x = read(t).astype(F32)
            y = x * inv * norm_gain[:, cols] * (1.0 + mods[t, 2 + row : 3 + row, :]) + mods[
                t, row : row + 1, :
            ]
            hidden[0:rows, cols] = y.astype(BF16)

    def headnorm(x, gain):
        width = x.shape[1]
        head = lax.broadcasted_iota(jnp.int32, x.shape, 1) // CHANNEL_SPAN
        sq = x * x
        scale = jnp.zeros_like(x)
        for h in range(width // CHANNEL_SPAN):
            s = jnp.sum(jnp.where(head == h, sq, 0.0), axis=-1, keepdims=True)
            scale = jnp.where(head == h, lax.rsqrt(s / CHANNEL_SPAN + epsilon), scale)
        return x * scale * gain

    def rotate(x, cos, sin):
        width = x.shape[1]
        full = x if width == 128 else jnp.concatenate([x, x], axis=1)
        lane = lax.broadcasted_iota(jnp.int32, full.shape, 1)
        other = jnp.where(lane % 32 < 16, pltpu.roll(full, 112, 1), pltpu.roll(full, 16, 1))
        return (full * cos + other * sin)[:, :width]

    piece = min(128, kv_width)
    q_pair = jnp.concatenate([q_gain[...], q_gain[...]], axis=1)
    k_pair = jnp.concatenate([k_gain[...], k_gain[...]], axis=1)

    def context_step():
        modulate(lambda t: context[:, t * span : (t + 1) * span], ctx_rows, 1)
        h = hidden[0:ctx_rows, :]
        k = jnp.dot(h, w_k[...], preferred_element_type=F32)
        for c in range(0, kv_width, piece):
            kv_out[0:ctx_rows, c : c + piece] = headnorm(
                k[:, c : c + piece], k_pair[:, :piece]
            ).astype(BF16)
        kv_out[0:ctx_rows, kv_width:] = jnp.dot(h, w_v[...], preferred_element_type=F32).astype(
            BF16
        )

    def tile(i):
        modulate(lambda t: lat_all[i, :, t * span : (t + 1) * span], own_rows, 0)
        h = hidden[0:own_rows, :]
        rows = pl.ds(pl.multiple_of(i * own_rows, own_rows), own_rows)
        cos, sin = cosine[rows, :], sine[rows, :]
        low = pl.ds(pl.multiple_of(ctx_rows + i * own_rows, 16), own_rows)
        k = jnp.dot(h, w_k[...], preferred_element_type=F32)
        for c in range(0, kv_width, piece):
            kv_out[low, c : c + piece] = rotate(
                headnorm(k[:, c : c + piece], k_pair[:, :piece]), cos, sin
            ).astype(BF16)
        kv_out[low, kv_width:] = jnp.dot(h, w_v[...], preferred_element_type=F32).astype(BF16)
        q = jnp.dot(h, w_q[...], preferred_element_type=F32)
        for c in range(0, q_width, 128):
            y = rotate(headnorm(q[:, c : c + 128], q_pair), cos, sin).astype(BF16)
            y = y.astype(F32) * CHANNEL_SPAN ** (-0.5)
            lane = lax.broadcasted_iota(jnp.int32, y.shape, 1)
            for j in range(2):
                head = c // CHANNEL_SPAN + j
                place = head // group
                moved = y if place % 2 == j else pltpu.roll(y, 64, 1)
                base = place // 2 * 128
                inside = lane // CHANNEL_SPAN == place % 2
                blank = jnp.where(inside, moved, 0.0).astype(BF16)
                for b in range(0, kv_width, piece):
                    q_out[head, rows, b : b + piece] = (
                        blank[:, :piece] if b == base else jnp.zeros((own_rows, piece), BF16)
                    )

    return context_step, tile


def attend_kernel(
    n_sp, n_tp, lows, tile_rows, unroll, ctx_rows, offset, q, kv, mods, latent_hbm, w_out_hbm, out,
    kv_all, peak, total, acc, attended, received, latent, w_out,
    lo_send, hi_send, fwd_send, kv_recv, at_send, at_recv, own_sem, lat_sem, w_sem,
):
    sp, tp = lax.axis_index("sp"), lax.axis_index("tp")
    tok, width2 = q.shape[1], kv.shape[1]
    width = width2 // 2
    kv_heads = width // CHANNEL_SPAN
    q_heads = q.shape[0]
    group = q_heads // kv_heads
    own_rows = tok // n_tp
    q_width = q_heads * CHANNEL_SPAN
    fetch = pltpu.make_async_copy(w_out_hbm, w_out, w_sem)
    fetch_latent = pltpu.make_async_copy(latent_hbm, latent, lat_sem)
    greet(n_sp, n_tp)
    highs = n_sp // lows
    low, high = lax.rem(sp, lows), sp // lows

    def copy(src, slot, send_sem, peer):
        return pltpu.make_async_remote_copy(
            src_ref=slot, dst_ref=kv_all.at[src], send_sem=send_sem,
            recv_sem=kv_recv.at[src], device_id=(peer, tp), device_id_type=MESH,
        )

    def low_peer(d):
        return high * lows + lax.rem(low + d, lows)

    def high_peer(d):
        return lax.rem(high + d, highs) * lows + low

    sends = [copy(sp, kv, lo_send.at[d - 1], low_peer(d)) for d in range(1, lows)]
    sends += [copy(sp, kv, hi_send.at[d - 1], high_peer(d)) for d in range(1, highs)]
    for c in sends:
        c.start()
    own = pltpu.make_async_copy(kv, kv_all.at[sp], own_sem)
    own.start()
    fetch.start()
    fetch_latent.start()
    tiles = tok // tile_rows

    def update(keys, values, shift, first):
        def step(i, carry):
            head, r = i // tiles, lax.rem(i, tiles)
            rows = pl.ds(pl.multiple_of(r * tile_rows, tile_rows), tile_rows)
            s = lax.dot_general(
                q[head, rows, :], keys(), (((1,), (1,)), ((), ())), preferred_element_type=F32
            )
            if shift:
                s = s + shift
            top = jnp.max(s, axis=-1, keepdims=True)
            if not first:
                old = peak[head, rows, 0:1]
                top = jnp.maximum(top, old)
                shrink = jnp.exp(old - top)
            e = jnp.exp(s - top)
            row_sum = e[:, 0:128]
            for c in range(128, e.shape[1], 128):
                row_sum = row_sum + e[:, c : c + 128]
            w = jnp.dot(e.astype(BF16), values(), preferred_element_type=F32)
            if not first:
                row_sum = row_sum + total[head, rows, :] * shrink
                w = w + acc[head, rows, :] * shrink
            peak[head, rows, :] = jnp.broadcast_to(top, (tile_rows, 128))
            total[head, rows, :] = row_sum
            acc[head, rows, :] = w
            return carry

        lax.fori_loop(0, q_heads * tiles, step, 0, unroll=unroll)

    def attend(src):
        update(
            lambda: kv_all[src, ctx_rows:, :width], lambda: kv_all[src, ctx_rows:, width:],
            0.0, False,
        )

    def arrive(src):
        copy(src, kv, lo_send.at[0], low_peer(0)).wait_recv()

    update(lambda: kv[ctx_rows:, :width], lambda: kv[ctx_rows:, width:], 0.0, True)

    def near(d, carry):
        src = high * lows + lax.rem(low - d + lows, lows)
        arrive(src)
        attend(src)
        return carry

    lax.fori_loop(1, lows, near, 0)

    def column(d, carry):
        row = lax.rem(high - d + highs, highs) * lows
        src = row + low
        arrive(src)

        def pass_on(e, inner):
            copy(
                src, kv_all.at[src], fwd_send.at[(d - 1) * (lows - 1) + e - 1], low_peer(e)
            ).start()
            return inner

        lax.fori_loop(1, lows, pass_on, 0)
        attend(src)
        return carry

    lax.fori_loop(1, highs, column, 0)

    def rest(k, carry):
        d, e = k // (lows - 1) + 1, lax.rem(k, lows - 1) + 1
        src = lax.rem(high - d + highs, highs) * lows + lax.rem(low - e + lows, lows)
        arrive(src)
        attend(src)
        return carry

    lax.fori_loop(0, (highs - 1) * (lows - 1), rest, 0)
    own.wait()
    ctx_count = n_sp * ctx_rows
    update(
        lambda: kv_all[:, :ctx_rows, :width].reshape(ctx_count, width),
        lambda: kv_all[:, :ctx_rows, width:].reshape(ctx_count, width),
        offset,
        False,
    )
    for c in sends:
        c.wait_send()

    def sent(k, carry):
        copy(sp, kv, fwd_send.at[k], low_peer(1)).wait_send()
        return carry

    lax.fori_loop(0, (highs - 1) * (lows - 1), sent, 0)
    for t in range(n_tp):
        rows = slice(t * own_rows, (t + 1) * own_rows)
        for h in range(q_heads):
            g = h // group
            a = acc[h, rows, :] / jnp.sum(total[h, rows, :], axis=-1, keepdims=True)
            attended[t, :, h * CHANNEL_SPAN : (h + 1) * CHANNEL_SPAN] = a[
                :, g * CHANNEL_SPAN : (g + 1) * CHANNEL_SPAN
            ].astype(BF16)
    copies = []
    for d in range(1, n_tp):
        peer = lax.rem(tp + d, n_tp)
        c = pltpu.make_async_remote_copy(
            src_ref=attended.at[peer], dst_ref=received.at[tp], send_sem=at_send.at[d - 1],
            recv_sem=at_recv.at[d - 1], device_id=(sp, peer), device_id_type=MESH,
        )
        c.start()
        copies.append(c)
    received[tp] = attended[tp]
    fetch.wait()
    fetch_latent.wait()
    for c in copies:
        c.wait()
    span = mods.shape[2]
    for t in range(n_tp):
        cols = slice(t * span, (t + 1) * span)
        branch = jnp.zeros((own_rows, span), F32)
        for s in range(n_tp):
            branch = branch + jnp.dot(
                received[s],
                w_out[s * q_width : (s + 1) * q_width, cols],
                preferred_element_type=F32,
            )
        out[:, cols] = (latent[:, cols].astype(F32) + mods[t, 4:5, :] * branch).astype(BF16)


def on_device(
    latent, context, condition, context_condition, norm_gain, shift_weight, scale_weight,
    gate_weight, query_weight, key_weight, value_weight, query_gain, key_gain, output_weight,
):
    n_sp, n_tp = lax.axis_size("sp"), lax.axis_size("tp")
    seq_index = lax.axis_index("sp")
    row_slab, columns = shift_weight.shape
    own_rows, model = latent.shape
    ctx_rows = context.shape[0]
    tok = own_rows * n_tp
    q_width, kv_width = query_weight.shape[1], key_weight.shape[1]
    q_heads = q_width // CHANNEL_SPAN
    conditions = jnp.stack([condition, context_condition])
    act = jax.nn.silu(
        lax.dynamic_slice_in_dim(conditions, seq_index * row_slab, row_slab, 1)
    ).astype(BF16)
    dma = pltpu.SemaphoreType.DMA
    quarter = CHANNEL_SPAN // 4
    lane = jnp.arange(128, dtype=jnp.int32) % CHANNEL_SPAN
    inverse = (rope_base ** (-(lane % quarter).astype(F32) / quarter))[None]
    anywhere = pl.BlockSpec(memory_space=pl.ANY)
    q, kv, mods = pl.pallas_call(
        functools.partial(gather_kernel, n_sp, n_tp),
        out_shape=(
            jax.ShapeDtypeStruct((q_heads, tok, kv_width), BF16),
            jax.ShapeDtypeStruct((ctx_rows + tok, 2 * kv_width), BF16),
            jax.ShapeDtypeStruct((n_tp, 8, columns), F32),
        ),
        in_specs=[anywhere, VMEM] + [anywhere] * 4 + [VMEM] + [anywhere] * 3 + [VMEM] * 3,
        out_specs=(VMEM, VMEM, VMEM),
        scratch_shapes=[
            pltpu.VMEM((n_tp, own_rows, model), BF16),
            pltpu.VMEM((3, row_slab, columns), BF16),
            pltpu.VMEM(context.shape, BF16),
            pltpu.VMEM(query_weight.shape, BF16),
            pltpu.VMEM(key_weight.shape, BF16),
            pltpu.VMEM(value_weight.shape, BF16),
            pltpu.VMEM((max(own_rows, ctx_rows), model), BF16),
            pltpu.VMEM((8, columns), F32),
            pltpu.VMEM((n_sp, 8, columns), F32),
            pltpu.VMEM((tok, 128), F32),
            pltpu.VMEM((tok, 128), F32),
            dma((8,)), dma((n_tp // 2,)), dma((n_tp,)), dma((max(n_tp // 2 - 1, 1),)),
            dma((n_sp - 1,)), dma((n_sp - 1,)), dma((n_tp - 1,)), dma((n_tp - 1,)),
        ],
        compiler_params=pltpu.CompilerParams(
            collective_id=0, has_side_effects=True, vmem_limit_bytes=56 << 20
        ),
        name="gather_project",
    )(
        latent, act, shift_weight, scale_weight, gate_weight, context, norm_gain[None],
        query_weight, key_weight, value_weight,
        query_gain[None], key_gain[None], inverse,
    )
    offset = math.log(tok / (2.0 * ctx_rows))
    tile_rows = math.gcd(tok, TILE)
    lows = 2 ** (int(math.log2(n_sp)) // 2)
    return pl.pallas_call(
        functools.partial(
            attend_kernel, n_sp, n_tp, lows, tile_rows, UNROLL, ctx_rows, offset
        ),
        out_shape=jax.ShapeDtypeStruct(latent.shape, BF16),
        in_specs=[VMEM] * 3 + [anywhere] * 2,
        out_specs=VMEM,
        scratch_shapes=[
            pltpu.VMEM((n_sp, ctx_rows + tok, 2 * kv_width), BF16),
            pltpu.VMEM((q_heads, tok, 128), F32),
            pltpu.VMEM((q_heads, tok, 128), F32),
            pltpu.VMEM((q_heads, tok, kv_width), F32),
            pltpu.VMEM((n_tp, own_rows, q_width), BF16),
            pltpu.VMEM((n_tp, own_rows, q_width), BF16),
            pltpu.VMEM(latent.shape, BF16),
            pltpu.VMEM(output_weight.shape, BF16),
            dma((lows - 1,)), dma((n_sp // lows - 1,)),
            dma(((n_sp // lows - 1) * (lows - 1),)), dma((n_sp,)),
            dma((n_tp - 1,)), dma((n_tp - 1,)), dma, dma, dma,
        ],
        compiler_params=pltpu.CompilerParams(
            collective_id=1, has_side_effects=True, vmem_limit_bytes=56 << 20
        ),
        name="attend",
    )(q, kv, mods, latent, output_weight)


def solution(mesh):
    in_specs = (
        P(("sp", "tp"), None), P("sp", None), P(), P(), P(),
        P("sp", "tp"), P("sp", "tp"), P("sp", "tp"),
        P(None, "tp"), P(None, "tp"), P(None, "tp"), P(), P(), P(),
    )
    return jax.shard_map(
        on_device, mesh=mesh, in_specs=in_specs, out_specs=P(("sp", "tp"), None), check_vma=False
    )
```
